32 devices in a mesh: grp: 2 (over y), sp: 4 (over z), tp: 4 (over x, core).
Axes of the slice: x: 2, y: 2, z: 4, core: 2. Of those that a mesh axis runs over, the one named last changes fastest.
Arguments:
- hidden_items: bfloat16 [1024, 4096], P(('grp', 'sp', 'tp')), parts along dimension 0, may hold values from -6 to 6
- sample_cond: bfloat16 [8192], P('grp'), parts along dimension 0, may hold values from -6 to 6
- prompt_items: bfloat16 [256, 4096], P(('grp', 'sp')), parts along dimension 0, may hold values from -6 to 6
- prompt_cond: bfloat16 [4096], replicated, may hold values from -6 to 6
- adjust_shifting: bfloat16 [4096, 4096], P('sp', 'tp'), may hold values from -0.125 to 0.125
- adjust_stretch: bfloat16 [4096, 4096], P('sp', 'tp'), may hold values from -0.125 to 0.125
- skip_valve: bfloat16 [4096, 4096], P('sp', 'tp'), may hold values from -0.125 to 0.125
- receiver_matrix: bfloat16 [4096, 2048], P(None, 'tp'), may hold values from -0.09375 to 0.09375
- address_matrix: bfloat16 [4096, 2048], P(None, 'tp'), may hold values from -0.09375 to 0.09375
- payload_matrix: bfloat16 [4096, 2048], P(None, 'tp'), may hold values from -0.09375 to 0.09375
- joint_lower_projector: bfloat16 [4096, 64], P('sp'), may hold values from -0.09375 to 0.09375
- fading_raise_matrix: bfloat16 [64, 2048], P(None, 'tp'), may hold values from -1.5 to 1.5
- step_raise_matrix: bfloat16 [64, 2048], P(None, 'tp'), may hold values from -1.5 to 1.5
- feature_fading: float32 [2048], P('tp'), may hold values from 0 to 0.1, as said below
- spike_logfade: float32 [1024, 32], P(('grp', 'sp'), 'tp'), parts along dimension 0, may hold values from 0 to 2
- group_standard_factor: float32 [2048], P('tp'), may hold values from 0.1 to 1.9
- emit_matrix: bfloat16 [2048, 4096], P('tp', 'sp'), may hold values from -0.125 to 0.125
Outputs:
- latent_out: bfloat16 [1024, 4096], P(('grp', 'sp', 'tp')), parts along dimension 0
The draws below stay inside these ranges and needn't reach their ends.
There are 2 independent parts, one for each index of `grp`. The reference program is written for one: setup_inputs(seed, part) draws one part's arguments, and reference() takes and returns one part's arrays. A program takes and returns all parts, laid end to end along the dimension named above; an argument that names none is the same for every part. Nothing has to cross between parts.
Inputs may be any that keep to these rules, and one draw needn't show every extreme that they name: `feature_fading`: per-token decay rate of each channel.
All inputs are finite; a program needn't handle non-finite values.
Results may differ from the reference program's by a relative error of at most 0.015.
Values may be sent and summed in bfloat16 or wider, within the bound.
A program may use at most 128 MiB of HBM per device.

```python
import math
import jax
import jax.numpy as jnp
from jax import lax

D = 4096
ATTEND_GROUPS = 32
ATTEND_WIDTH = 64
RANK = 64
TOK_SP = 128
CTX = 128
HIDDEN_COUNT = 512
A_WIDTH = 2048
N_TP = 4


def draw_feature_fading(key, part):
    key_one, another_address, further_address = jax.random.split(jax.random.fold_in(key, 11), 3)
    chain_len = HIDDEN_COUNT + CTX
    quick_heads = jax.random.randint(key_one, (ATTEND_GROUPS,), 0, 2) == 0
    fast_rate = jnp.exp(jax.random.uniform(another_address, (ATTEND_GROUPS, ATTEND_WIDTH), jnp.float32, math.log(0.035), math.log(0.09)))
    slow_rate = jnp.exp(jax.random.uniform(further_address, (ATTEND_GROUPS, ATTEND_WIDTH), jnp.float32, math.log(0.2), math.log(1.0))) / chain_len
    return jnp.where(quick_heads[:, None], fast_rate, slow_rate).reshape(ATTEND_GROUPS * ATTEND_WIDTH).astype(jnp.float32)


def draw_spike_logfade(key, part):
    key_one, another_address, further_address = jax.random.split(jax.random.fold_in(key, 23), 3)
    chain_len = HIDDEN_COUNT + CTX
    block_count = HIDDEN_COUNT // TOK_SP
    levels = jnp.exp(jax.random.uniform(key_one, (block_count, 1, ATTEND_GROUPS), jnp.float32, math.log(0.1), math.log(1.0))) / chain_len
    drawn_answer = jnp.broadcast_to(levels, (block_count, TOK_SP, ATTEND_GROUPS)).reshape(HIDDEN_COUNT, ATTEND_GROUPS)
    spike_places = jax.random.randint(another_address, (2, ATTEND_GROUPS), 0, HIDDEN_COUNT)
    spike_span = -jnp.log(jax.random.uniform(further_address, (2, ATTEND_GROUPS), jnp.float32, 0.5, 0.8))
    agreement_marks = jnp.arange(HIDDEN_COUNT)[:, None, None] == spike_places[None]
    spike_present = jnp.sum(jnp.where(agreement_marks, spike_span[None], 0.0), axis=1)
    return (drawn_answer + spike_present).astype(jnp.float32)


def block_levels(stream_key, dims, cuts, least, high):
    def one(dim, shards_of):
        steps = jax.random.uniform(jax.random.fold_in(jax.random.fold_in(stream_key, 6), dim), (shards_of,), jnp.float32, least / len(cuts), high / len(cuts))
        return jnp.repeat(jnp.exp(steps), dims[dim] // shards_of).reshape((-1,) + (1,) * (len(dims) - dim - 1))

    level = one(*cuts[0])
    for cut in cuts[1:]:
        level = level * one(*cut)
    return level


def bell_draw(key, dims, deviation, bound, cuts=(), kind=jnp.bfloat16):
    array = jax.random.normal(key, dims, jnp.float32) * deviation
    if len(cuts) > 0:
        array = block_levels(key, dims, cuts, -0.22, 0.18) * array
    return jnp.clip(array, min=-bound, max=bound).astype(kind)


def setup_inputs(seed: int = 0, part: int = 0) -> dict:
    keys = jax.random.split(jax.random.key(seed), 18)
    part_splits = jax.random.split(jax.random.fold_in(keys[17], part), 18)
    return {
        "hidden_items": bell_draw(part_splits[0], (HIDDEN_COUNT, D), 1.0, 6.0, ((0, 16),)),
        "sample_cond": bell_draw(part_splits[1], (D,), 1.0, 6.0),
        "prompt_items": bell_draw(part_splits[2], (CTX, D), 1.0, 6.0, ((0, 4),)),
        "prompt_cond": bell_draw(keys[3], (D,), 1.0, 6.0),
        "adjust_shifting": bell_draw(keys[4], (D, D), (D // 2) ** -0.5, 0.125, ((0, 4), (1, 4))),
        "adjust_stretch": bell_draw(keys[5], (D, D), (D // 2) ** -0.5, 0.125, ((0, 4), (1, 4))),
        "skip_valve": bell_draw(keys[6], (D, D), (D // 2) ** -0.5, 0.125, ((0, 4), (1, 4))),
        "receiver_matrix": bell_draw(keys[7], (D, A_WIDTH), D ** -0.5, 0.09375, ((1, 4),)),
        "address_matrix": bell_draw(keys[8], (D, A_WIDTH), D ** -0.5, 0.09375, ((1, 4),)),
        "payload_matrix": bell_draw(keys[9], (D, A_WIDTH), D ** -0.5, 0.09375, ((1, 4),)),
        "joint_lower_projector": bell_draw(keys[10], (D, RANK), D ** -0.5, 0.09375, ((0, 4),)),
        "fading_raise_matrix": bell_draw(keys[11], (RANK, A_WIDTH), 0.25, 1.5, ((1, 4),)),
        "step_raise_matrix": bell_draw(keys[12], (RANK, A_WIDTH), (RANK // 4) ** -0.5, 1.5, ((1, 4),)),
        "feature_fading": draw_feature_fading(jax.random.fold_in(keys[17], 71), part),
        "spike_logfade": draw_spike_logfade(jax.random.fold_in(jax.random.fold_in(keys[17], part), 71), part),
        "group_standard_factor": jnp.clip(1.0 + 0.18 * jax.random.normal(keys[15], (A_WIDTH,), jnp.float32), 0.1, 1.9),
        "emit_matrix": bell_draw(keys[16], (A_WIDTH, D), A_WIDTH ** -0.5, 0.125, ((0, 4), (1, 4))),
    }


EXACT_MODE = lax.Precision.HIGHEST
rate_shift = 5.0

def stored(value):
    return lax.optimization_barrier(value.astype(jnp.bfloat16))

def product(left, right):
    return jnp.dot(left, right, preferred_element_type=jnp.float32)

def modulate(rows, shifts, scales):
    values = rows.astype(jnp.float32)
    centre = lax.optimization_barrier(jnp.mean(values, -1, keepdims=True))
    spread = lax.optimization_barrier(jnp.mean(jnp.square(values - centre), -1, keepdims=True))
    normed = (values - centre) * lax.rsqrt(spread + 1e-05)
    return (normed * (1.0 + scales) + shifts).astype(jnp.bfloat16)

def head_inputs(u_rows, address_matrix, payload_matrix, joint_lower_projector, fading_raise_matrix, step_raise_matrix, feature_fading, surplus_entries):
    row_count = u_rows.shape[0]
    key_rows = stored(product(u_rows, address_matrix))
    value_rows = stored(product(u_rows, payload_matrix))
    low_rows = stored(product(u_rows, joint_lower_projector))
    squashed = jnp.tanh(low_rows.astype(jnp.float32)).astype(jnp.bfloat16)
    logdecay = -feature_fading * jax.nn.sigmoid(product(squashed, fading_raise_matrix)) - surplus_entries
    learned = jax.nn.sigmoid(product(squashed, step_raise_matrix) - rate_shift)
    key_heads = key_rows.astype(jnp.float32).reshape(row_count, ATTEND_GROUPS, ATTEND_WIDTH)
    unit_keys = key_heads * lax.rsqrt(lax.optimization_barrier(jnp.sum(key_heads * key_heads, -1, keepdims=True)) + 1e-06)
    removal = unit_keys * learned.reshape(row_count, ATTEND_GROUPS, ATTEND_WIDTH)
    retain = jnp.exp(logdecay).reshape(row_count, ATTEND_GROUPS, ATTEND_WIDTH)
    value_heads = value_rows.astype(jnp.float32).reshape(row_count, ATTEND_GROUPS, ATTEND_WIDTH)
    return (retain, key_heads, value_heads, unit_keys, removal)

def advance(carried, inputs):
    retain, key_heads, value_heads, unit_keys, removal = inputs
    probed = jnp.einsum('hvk,hk->hv', carried, unit_keys, precision=EXACT_MODE)
    return carried * retain[:, None, :] - probed[:, :, None] * removal[:, None, :] + value_heads[:, :, None] * key_heads[:, None, :]

def step_plain(carried, inputs):
    return (advance(carried, inputs), jnp.zeros((), jnp.float32))

def step_read(carried, inputs):
    carried = advance(carried, inputs[:5])
    return (carried, jnp.einsum('hvk,hk->hv', carried, inputs[5], precision=EXACT_MODE))

def reference(hidden_items, sample_cond, prompt_items, prompt_cond, adjust_shifting, adjust_stretch, skip_valve, receiver_matrix, address_matrix, payload_matrix, joint_lower_projector, fading_raise_matrix, step_raise_matrix, feature_fading, spike_logfade, group_standard_factor, emit_matrix):
    activated = jax.nn.silu(jnp.stack([sample_cond, prompt_cond]).astype(jnp.float32)).astype(jnp.bfloat16)
    shifts = product(activated, adjust_shifting)
    scales = product(activated, adjust_stretch)
    gates = product(activated[:1], skip_valve)[0]
    u_latent = modulate(hidden_items, shifts[0], scales[0])
    u_context = modulate(prompt_items, shifts[1], scales[1])
    query_heads = stored(product(u_latent, receiver_matrix)).astype(jnp.float32).reshape(HIDDEN_COUNT, ATTEND_GROUPS, ATTEND_WIDTH)
    surplus_entries = jnp.repeat(spike_logfade, ATTEND_WIDTH, axis=1)
    latent_parts = head_inputs(u_latent, address_matrix, payload_matrix, joint_lower_projector, fading_raise_matrix, step_raise_matrix, feature_fading, surplus_entries)
    context_parts = head_inputs(u_context, address_matrix, payload_matrix, joint_lower_projector, fading_raise_matrix, step_raise_matrix, feature_fading, 0.0)
    zeroed = jnp.zeros((ATTEND_GROUPS, ATTEND_WIDTH, ATTEND_WIDTH), jnp.float32)
    ctx_forward, _ = lax.scan(step_plain, zeroed, context_parts)
    ctx_backward, _ = lax.scan(step_plain, zeroed, context_parts, reverse=True)
    _, forward = lax.scan(step_read, ctx_forward, latent_parts + (query_heads,))
    _, backward = lax.scan(step_read, ctx_backward, latent_parts + (query_heads,), reverse=True)
    combined = forward + backward
    centre = lax.optimization_barrier(jnp.mean(combined, -1, keepdims=True))
    spread = lax.optimization_barrier(jnp.mean(jnp.square(combined - centre), -1, keepdims=True))
    normed = (combined - centre) * lax.rsqrt(spread + 0.00064) * group_standard_factor.reshape(ATTEND_GROUPS, ATTEND_WIDTH)
    normed = normed.reshape(HIDDEN_COUNT, ATTEND_GROUPS * ATTEND_WIDTH).astype(jnp.bfloat16)
    stride = ATTEND_GROUPS * ATTEND_WIDTH // N_TP
    mixed_sum = jnp.zeros((HIDDEN_COUNT, D), jnp.float32)
    for number in range(N_TP):
        portion = product(normed[:, number * stride:(number + 1) * stride], emit_matrix[number * stride:(number + 1) * stride])
        mixed_sum = mixed_sum + lax.optimization_barrier(portion.astype(jnp.bfloat16)).astype(jnp.float32)
    return (hidden_items.astype(jnp.float32) + gates * mixed_sum).astype(jnp.bfloat16)
```

```python
import functools
import math

import jax
import jax.numpy as jnp
from jax import lax
from jax.experimental import pallas as pl
from jax.experimental.pallas import tpu as pltpu
from jax.sharding import PartitionSpec as P

ATTEND_WIDTH = 64
PAIR = 2 * ATTEND_WIDTH

EXACT_MODE = lax.Precision.HIGHEST
EPS_ROW = 1e-05
EPS_HEAD = 0.00064
EPS_KEY = 1e-06
rate_shift = 5.0


def stored(value):
    return lax.optimization_barrier(value.astype(jnp.bfloat16))


def product(left, right):
    return jnp.dot(left, right, preferred_element_type=jnp.float32)


def modulate(rows, shifts, scales):
    values = rows.astype(jnp.float32)
    centre = jnp.mean(values, -1, keepdims=True)
    spread = jnp.mean(jnp.square(values - centre), -1, keepdims=True)
    normed = (values - centre) * lax.rsqrt(spread + EPS_ROW)
    return (normed * (1.0 + scales) + shifts).astype(jnp.bfloat16)


def low_dot(left, right):
    return jnp.dot(
        left.astype(jnp.bfloat16), right.astype(jnp.bfloat16), preferred_element_type=jnp.float32
    )


def low_dot_nt(left, right):
    return lax.dot_general(
        left.astype(jnp.bfloat16),
        right.astype(jnp.bfloat16),
        (((1,), (1,)), ((), ())),
        preferred_element_type=jnp.float32,
    )


def low_dot_tn(left, right):
    return lax.dot_general(
        left.astype(jnp.bfloat16),
        right.astype(jnp.bfloat16),
        (((0,), (0,)), ((), ())),
        preferred_element_type=jnp.float32,
    )


def exact_dot(left, right):
    return jnp.dot(left, right, precision=EXACT_MODE, preferred_element_type=jnp.float32)


def head_mask(size):
    row = lax.broadcasted_iota(jnp.int32, (size, size), 0)
    col = lax.broadcasted_iota(jnp.int32, (size, size), 1)
    return (row // ATTEND_WIDTH) == (col // ATTEND_WIDTH)


def token_features(keys, lows, raise_fading, raise_step, fading):
    squashed = jnp.tanh(lows.astype(jnp.float32)).astype(jnp.bfloat16)
    logdecay = -fading * jax.nn.sigmoid(product(squashed, raise_fading))
    learned = jax.nn.sigmoid(product(squashed, raise_step) - rate_shift)
    same_head = head_mask(PAIR).astype(jnp.float32)
    unit = keys * lax.rsqrt(exact_dot(keys * keys, same_head) + EPS_KEY)
    return unit, unit * learned, logdecay


def block_inverses(systems, uppers):
    size = systems[0].shape[0]
    row = lax.broadcasted_iota(jnp.int32, (size, size), 0)
    col = lax.broadcasted_iota(jnp.int32, (size, size), 1)
    eye = (row == col).astype(jnp.float32)
    inverses = None
    width = 1
    while width < size:
        merged = (row // (2 * width) == col // (2 * width)) & (row // width != col // width)
        pieces = [jnp.where(merged, system, 0.0) for system in systems]
        if inverses is None:
            inverses = [eye - piece for piece in pieces]
        else:
            firsts = [low_dot(inverse, piece) for inverse, piece in zip(inverses, pieces)]
            inverses = [
                inverse - low_dot(first, inverse) for first, inverse in zip(firsts, inverses)
            ]
        width *= 2
    return inverses


def chain_terms(parts, spike_pair, spike_rows, queries):
    unit, removal, logdecay, keys, values = parts
    size = keys.shape[0]
    row = lax.broadcasted_iota(jnp.int32, (size, size), 0)
    col = lax.broadcasted_iota(jnp.int32, (size, size), 1)
    lane = lax.broadcasted_iota(jnp.int32, (1, PAIR), 1)
    first_head = lane < ATTEND_WIDTH
    upto = (row >= col).astype(jnp.float32)
    ahead = exact_dot(upto, logdecay)
    behind = ahead[-1:, :] - ahead + logdecay
    if spike_pair is not None:
        spike_ahead = exact_dot(upto, spike_pair)
        spike_behind = spike_ahead[-1:, :] - spike_ahead + spike_pair
        rows_ahead = exact_dot(spike_rows, (row <= col).astype(jnp.float32))
        rows_behind = exact_dot(spike_rows, (row >= col).astype(jnp.float32))
    out = []
    for upper in (False, True):
        totals = behind if upper else ahead
        whole = totals[:1, :] if upper else totals[-1:, :]
        inverse = jnp.exp(-totals)
        exclusive = jnp.exp(totals - logdecay)
        probed = exclusive * unit
        key_in = keys * inverse
        removal_in = removal * inverse
        left = [probed]
        tail = whole - totals
        probed_start = probed
        if spike_pair is not None:
            sp_tot = spike_behind if upper else spike_ahead
            sp_whole = sp_tot[:1, :] if upper else sp_tot[-1:, :]
            sp_row = rows_behind if upper else rows_ahead
            tail = tail + sp_whole - sp_tot
            whole = whole + sp_whole
            probed_start = unit * jnp.exp(totals - logdecay + sp_tot - spike_pair)
        tail = jnp.exp(tail)
        if queries is not None:
            weighted = jnp.exp(totals) * queries
            left.append(weighted)
            weighted_start = weighted
            if spike_pair is not None:
                weighted_start = queries * jnp.exp(totals + sp_tot)
        else:
            weighted_start = None
        strict = (row < col) if upper else (row > col)
        reach = (row <= col) if upper else (row >= col)
        right = jnp.concatenate([removal_in, key_in], axis=0)
        left = jnp.concatenate(left, axis=0)
        heads = []
        for number in range(2):
            own = first_head if number == 0 else jnp.logical_not(first_head)
            scores = low_dot_nt(jnp.where(own, left, 0.0), right)
            cols = slice(number * ATTEND_WIDTH, number * ATTEND_WIDTH + 1)
            if spike_pair is not None:
                shift = sp_tot[:, cols] - sp_row[number : number + 1, :]
                strict_fade = jnp.exp(jnp.minimum(shift - spike_pair[:, cols], 0.0))
                reach_fade = jnp.exp(jnp.minimum(shift, 0.0))
            else:
                strict_fade = reach_fade = 1.0
            system = jnp.where(strict, scores[:size, :size] * strict_fade, 0.0)
            inflow = jnp.where(strict, scores[:size, size:] * strict_fade, 0.0)
            if queries is not None:
                read_back = jnp.where(reach, scores[size:, :size] * reach_fade, 0.0)
                read_in = jnp.where(reach, scores[size:, size:] * reach_fade, 0.0)
            else:
                read_back = read_in = None
            heads.append((system, inflow, read_back, read_in))
        out.append(
            dict(
                heads=heads,
                probed_start=probed_start,
                weighted_start=weighted_start,
                keys_out=keys * tail,
                removal_out=removal * tail,
                final=jnp.exp(whole),
            )
        )
    return out


def pick(first_head, pair):
    return jnp.where(first_head, pair[0], pair[1])


def folded(block):
    kept = jnp.where(head_mask(PAIR), block, 0.0)
    return kept[:ATTEND_WIDTH] + kept[ATTEND_WIDTH:]


def unfolded(pair):
    return jnp.where(head_mask(PAIR), jnp.concatenate([pair, pair], axis=0), 0.0)


def chain_kernel(
    query_ref,
    key_ref,
    value_ref,
    low_ref,
    ctx_key_ref,
    ctx_value_ref,
    ctx_low_ref,
    raise_fading_ref,
    raise_step_ref,
    fading_ref,
    spike_ref,
    spike_row_ref,
    maps_ref,
    ctx_ref,
    reading_ref,
    inside_ref,
):
    lane = lax.broadcasted_iota(jnp.int32, (1, PAIR), 1)
    first_head = lane < ATTEND_WIDTH
    shared = (raise_fading_ref[...], raise_step_ref[...], fading_ref[...])
    keys = key_ref[...].astype(jnp.float32)
    values = value_ref[...].astype(jnp.float32)
    parts = token_features(keys, low_ref[...], *shared) + (keys, values)
    latent = chain_terms(
        parts, -spike_ref[...], -spike_row_ref[0], query_ref[...].astype(jnp.float32)
    )
    ctx_keys = ctx_key_ref[...].astype(jnp.float32)
    ctx_values = ctx_value_ref[...].astype(jnp.float32)
    ctx_parts = token_features(ctx_keys, ctx_low_ref[...], *shared) + (ctx_keys, ctx_values)
    context = chain_terms(ctx_parts, None, None, None)
    inverses = block_inverses([head[0] for terms in latent for head in terms["heads"]], None)
    ctx_inverses = block_inverses([head[0] for terms in context for head in terms["heads"]], None)
    inside = None
    for way in range(2):
        terms = latent[way]
        inverse = inverses[2 * way : 2 * way + 2]
        flow = pick(first_head, [low_dot(head[1], values) for head in terms["heads"]])
        joined = jnp.concatenate([terms["probed_start"], flow], axis=1)
        solved = [low_dot(one, joined) for one in inverse]
        on_state = pick(first_head, [one[:, :PAIR] for one in solved])
        alone = pick(first_head, [one[:, PAIR:] for one in solved])
        both = jnp.concatenate([on_state, alone], axis=1)
        back = [low_dot(head[2], both) for head in terms["heads"]]
        read = pick(first_head, [low_dot(head[3], values) for head in terms["heads"]])
        reading_ref[way] = (
            terms["weighted_start"] - pick(first_head, [one[:, :PAIR] for one in back])
        ).astype(reading_ref.dtype)
        part = read - pick(first_head, [one[:, PAIR:] for one in back])
        inside = part if inside is None else inside + part
        crossed = low_dot_tn(both, terms["removal_out"])
        eye = lax.broadcasted_iota(jnp.int32, (PAIR, PAIR), 0) == lax.broadcasted_iota(
            jnp.int32, (PAIR, PAIR), 1
        )
        factor = jnp.where(eye, terms["final"], 0.0) - crossed[:PAIR]
        offset = low_dot_tn(values, terms["keys_out"]) - crossed[PAIR:]
        maps_ref[way, 0, 0] = folded(factor).astype(maps_ref.dtype)
        maps_ref[way, 0, 1] = folded(offset).astype(maps_ref.dtype)
        ctx_terms = context[way]
        ctx_inverse = ctx_inverses[2 * way : 2 * way + 2]
        flow = pick(first_head, [low_dot(head[1], ctx_values) for head in ctx_terms["heads"]])
        alone = pick(first_head, [low_dot(one, flow) for one in ctx_inverse])
        ctx_ref[way, 0] = folded(
            low_dot_tn(ctx_values, ctx_terms["keys_out"])
            - low_dot_tn(alone, ctx_terms["removal_out"])
        )
    inside_ref[...] = inside


def chain_call(
    query, key, value, low, ctx_key, ctx_value, ctx_low, raise_fading, raise_step, fading, spike
):
    rows, width = key.shape
    ctx_rows = ctx_key.shape[0]
    pairs = width // PAIR
    rank = low.shape[1]
    spike_pair = jnp.repeat(spike, ATTEND_WIDTH, axis=1)
    spike_rows = jnp.transpose(spike).reshape(pairs, 2, rows)
    columns = lambda height: pl.BlockSpec((height, PAIR), lambda i: (0, i))
    entire = lambda height: pl.BlockSpec((height, rank), lambda i: (0, 0))
    return pl.pallas_call(
        chain_kernel,
        grid=(pairs,),
        in_specs=[
            columns(rows),
            columns(rows),
            columns(rows),
            entire(rows),
            columns(ctx_rows),
            columns(ctx_rows),
            entire(ctx_rows),
            columns(rank),
            columns(rank),
            columns(1),
            columns(rows),
            pl.BlockSpec((1, 2, rows), lambda i: (i, 0, 0)),
        ],
        out_specs=[
            pl.BlockSpec((2, 1, 2, ATTEND_WIDTH, PAIR), lambda i: (0, i, 0, 0, 0)),
            pl.BlockSpec((2, 1, ATTEND_WIDTH, PAIR), lambda i: (0, i, 0, 0)),
            pl.BlockSpec((2, rows, PAIR), lambda i: (0, 0, i)),
            columns(rows),
        ],
        out_shape=[
            jax.ShapeDtypeStruct((2, pairs, 2, ATTEND_WIDTH, PAIR), jnp.bfloat16),
            jax.ShapeDtypeStruct((2, pairs, ATTEND_WIDTH, PAIR), jnp.float32),
            jax.ShapeDtypeStruct((2, rows, width), jnp.bfloat16),
            jax.ShapeDtypeStruct((rows, width), jnp.float32),
        ],
        compiler_params=pltpu.CompilerParams(dimension_semantics=("arbitrary",)),
        cost_estimate=pl.CostEstimate(
            flops=pairs * 8 * 17 * 2 * PAIR**3, bytes_accessed=4 << 20, transcendentals=0
        ),
    )(
        query,
        key,
        value,
        low,
        ctx_key,
        ctx_value,
        ctx_low,
        raise_fading,
        raise_step,
        fading.reshape(1, width),
        spike_pair,
        spike_rows,
    )


def read_kernel(own_ref, maps_ref, ctx_ref, reading_ref, inside_ref, gains_ref, normed_ref):
    shards = maps_ref.shape[0]
    pairs = maps_ref.shape[2]
    own = own_ref[0]
    same_head = head_mask(PAIR).astype(jnp.float32) * (1.0 / ATTEND_WIDTH)
    states = [
        [unfolded(ctx_ref[way, pair]) for pair in range(pairs)] for way in range(2)
    ]
    for number in range(shards - 1):
        for way in range(2):
            source = number if way == 0 else shards - 1 - number
            passed = (number < own) if way == 0 else (source > own)
            for pair in range(pairs):
                factor = unfolded(maps_ref[source, way, pair, 0].astype(jnp.float32))
                offset = unfolded(maps_ref[source, way, pair, 1].astype(jnp.float32))
                state = states[way][pair]
                states[way][pair] = jnp.where(passed, low_dot(state, factor) + offset, state)
    for pair in range(pairs):
        cols = slice(pair * PAIR, (pair + 1) * PAIR)
        combined = (
            inside_ref[:, cols]
            + low_dot_nt(reading_ref[0, :, cols], states[0][pair])
            + low_dot_nt(reading_ref[1, :, cols], states[1][pair])
        )
        centred = combined - exact_dot(combined, same_head)
        spread = exact_dot(centred * centred, same_head)
        normed = centred * lax.rsqrt(spread + EPS_HEAD) * gains_ref[:, cols]
        normed_ref[:, cols] = normed.astype(normed_ref.dtype)


def read_call(own, maps, ctx, reading, inside, gains):
    rows, width = inside.shape
    vmem = pl.BlockSpec(memory_space=pltpu.VMEM)
    return pl.pallas_call(
        read_kernel,
        in_specs=[pl.BlockSpec(memory_space=pltpu.SMEM)] + [vmem] * 5,
        out_specs=vmem,
        out_shape=jax.ShapeDtypeStruct((rows, width), jnp.bfloat16),
        cost_estimate=pl.CostEstimate(
            flops=8 * 4 * 2 * PAIR**3, bytes_accessed=4 << 20, transcendentals=0
        ),
    )(own.reshape(1), maps, ctx, reading, inside, gains.reshape(1, width))


def body(
    hidden_items,
    sample_cond,
    prompt_items,
    prompt_cond,
    adjust_shifting,
    adjust_stretch,
    skip_valve,
    receiver_matrix,
    address_matrix,
    payload_matrix,
    joint_lower_projector,
    fading_raise_matrix,
    step_raise_matrix,
    feature_fading,
    spike_logfade,
    group_standard_factor,
    emit_matrix,
):
    span_rows = adjust_shifting.shape[0]
    conditions = jnp.stack([sample_cond, prompt_cond])
    activated = jax.nn.silu(conditions.astype(jnp.float32)).astype(jnp.bfloat16)
    own_cols = lax.dynamic_slice_in_dim(activated, lax.axis_index("sp") * span_rows, span_rows, 1)
    partial = jnp.concatenate(
        [
            product(own_cols, adjust_shifting),
            product(own_cols, adjust_stretch),
            product(own_cols[:1], skip_valve),
        ],
        axis=0,
    )
    gathered = lax.all_gather(partial, ("sp", "tp"), axis=0, tiled=False)
    sp_count, tp_count = lax.axis_size("sp"), lax.axis_size("tp")
    gathered = gathered.reshape((sp_count, tp_count) + partial.shape)
    vectors = jnp.sum(gathered, axis=0)
    vectors = jnp.transpose(vectors, (1, 0, 2)).reshape(partial.shape[0], -1)
    shifts, scales, gates = vectors[:2], vectors[2:4], vectors[4:]
    down_weight = lax.all_gather(joint_lower_projector, "sp", axis=0, tiled=True)
    out_weight = lax.all_gather(emit_matrix, "sp", axis=1, tiled=True)
    u_rows = modulate(hidden_items, shifts[0], scales[0])
    features = lax.all_gather(u_rows, "tp", axis=0, tiled=True)
    ctx_mod = modulate(prompt_items, shifts[1], scales[1])
    rows = features.shape[0]
    both = jnp.concatenate([features, ctx_mod], axis=0)
    key = stored(product(both, address_matrix))
    value = stored(product(both, payload_matrix))
    low = stored(product(both, down_weight))
    query = stored(product(features, receiver_matrix))
    head_cols = key.shape[1]
    ctx_joined = jnp.concatenate([key[rows:], value[rows:], low[rows:]], axis=1)
    ctx_joined = lax.all_gather(ctx_joined, "sp", axis=0, tiled=True)
    maps, ctx_state, reading, inside = chain_call(
        query,
        key[:rows],
        value[:rows],
        low[:rows],
        ctx_joined[:, :head_cols],
        ctx_joined[:, head_cols : 2 * head_cols],
        ctx_joined[:, 2 * head_cols :],
        fading_raise_matrix,
        step_raise_matrix,
        feature_fading,
        spike_logfade,
    )
    every = lax.all_gather(maps, "sp", axis=0, tiled=False)
    normed = read_call(
        lax.axis_index("sp"), every, ctx_state, reading, inside, group_standard_factor
    )
    mixed_sum = lax.psum_scatter(
        product(normed, out_weight).astype(jnp.bfloat16), "tp", scatter_dimension=0, tiled=True
    ).astype(jnp.float32)
    return (hidden_items.astype(jnp.float32) + gates[0] * mixed_sum).astype(jnp.bfloat16)


def solution(mesh):
    placed = (
        P(("grp", "sp", "tp"), None),
        P("grp"),
        P(("grp", "sp"), None),
        P(),
        P("sp", "tp"),
        P("sp", "tp"),
        P("sp", "tp"),
        P(None, "tp"),
        P(None, "tp"),
        P(None, "tp"),
        P("sp", None),
        P(None, "tp"),
        P(None, "tp"),
        P("tp"),
        P(("grp", "sp"), "tp"),
        P("tp"),
        P("tp", "sp"),
    )
    return jax.shard_map(
        body, mesh=mesh, in_specs=placed, out_specs=P(("grp", "sp", "tp"), None), check_vma=False
    )
```

```python
import functools
import math

import jax
import jax.numpy as jnp
from jax import lax
from jax.experimental import pallas as pl
from jax.experimental.pallas import tpu as pltpu
from jax.sharding import PartitionSpec as P

ATTEND_WIDTH = 64
PAIR = 2 * ATTEND_WIDTH

EXACT_MODE = lax.Precision.HIGHEST
EPS_ROW = 1e-05
EPS_HEAD = 0.00064
EPS_KEY = 1e-06
rate_shift = 5.0


def stored(value):
    return lax.optimization_barrier(value.astype(jnp.bfloat16))


def product(left, right):
    return jnp.dot(left, right, preferred_element_type=jnp.float32)


def modulate(rows, shifts, scales):
    values = rows.astype(jnp.float32)
    centre = jnp.mean(values, -1, keepdims=True)
    spread = jnp.mean(jnp.square(values - centre), -1, keepdims=True)
    normed = (values - centre) * lax.rsqrt(spread + EPS_ROW)
    return (normed * (1.0 + scales) + shifts).astype(jnp.bfloat16)


def low_dot(left, right):
    return jnp.dot(
        left.astype(jnp.bfloat16), right.astype(jnp.bfloat16), preferred_element_type=jnp.float32
    )


def low_dot_nt(left, right):
    return lax.dot_general(
        left.astype(jnp.bfloat16),
        right.astype(jnp.bfloat16),
        (((1,), (1,)), ((), ())),
        preferred_element_type=jnp.float32,
    )


def low_dot_tn(left, right):
    return lax.dot_general(
        left.astype(jnp.bfloat16),
        right.astype(jnp.bfloat16),
        (((0,), (0,)), ((), ())),
        preferred_element_type=jnp.float32,
    )


def exact_dot(left, right):
    return jnp.dot(left, right, precision=EXACT_MODE, preferred_element_type=jnp.float32)


def head_mask(size):
    row = lax.broadcasted_iota(jnp.int32, (size, size), 0)
    col = lax.broadcasted_iota(jnp.int32, (size, size), 1)
    return (row // ATTEND_WIDTH) == (col // ATTEND_WIDTH)


def token_features(keys, lows, raise_fading, raise_step, fading):
    squashed = jnp.tanh(lows.astype(jnp.float32)).astype(jnp.bfloat16)
    logdecay = -fading * jax.nn.sigmoid(product(squashed, raise_fading))
    learned = jax.nn.sigmoid(product(squashed, raise_step) - rate_shift)
    same_head = head_mask(PAIR).astype(jnp.float32)
    unit = keys * lax.rsqrt(exact_dot(keys * keys, same_head) + EPS_KEY)
    return unit, unit * learned, logdecay


def block_inverses(systems, uppers):
    size = systems[0].shape[0]
    row = lax.broadcasted_iota(jnp.int32, (size, size), 0)
    col = lax.broadcasted_iota(jnp.int32, (size, size), 1)
    eye = (row == col).astype(jnp.float32)
    inverses = None
    width = 1
    while width < size:
        merged = (row // (2 * width) == col // (2 * width)) & (row // width != col // width)
        pieces = [jnp.where(merged, system, 0.0) for system in systems]
        if inverses is None:
            inverses = [eye - piece for piece in pieces]
        else:
            firsts = [low_dot(inverse, piece) for inverse, piece in zip(inverses, pieces)]
            inverses = [
                inverse - low_dot(first, inverse) for first, inverse in zip(firsts, inverses)
            ]
        width *= 2
    return inverses


def chain_terms(parts, spike_pair, spike_rows, queries):
    unit, removal, logdecay, keys, values = parts
    size = keys.shape[0]
    row = lax.broadcasted_iota(jnp.int32, (size, size), 0)
    col = lax.broadcasted_iota(jnp.int32, (size, size), 1)
    lane = lax.broadcasted_iota(jnp.int32, (1, PAIR), 1)
    first_head = lane < ATTEND_WIDTH
    upto = (row >= col).astype(jnp.float32)
    ahead = exact_dot(upto, logdecay)
    behind = ahead[-1:, :] - ahead + logdecay
    if spike_pair is not None:
        spike_ahead = exact_dot(upto, spike_pair)
        spike_behind = spike_ahead[-1:, :] - spike_ahead + spike_pair
        rows_ahead = exact_dot(spike_rows, (row <= col).astype(jnp.float32))
        rows_behind = exact_dot(spike_rows, (row >= col).astype(jnp.float32))
    out = []
    for upper in (False, True):
        totals = behind if upper else ahead
        whole = totals[:1, :] if upper else totals[-1:, :]
        inverse = jnp.exp(-totals)
        exclusive = jnp.exp(totals - logdecay)
        probed = exclusive * unit
        key_in = keys * inverse
        removal_in = removal * inverse
        left = [probed]
        tail = whole - totals
        probed_start = probed
        if spike_pair is not None:
            sp_tot = spike_behind if upper else spike_ahead
            sp_whole = sp_tot[:1, :] if upper else sp_tot[-1:, :]
            sp_row = rows_behind if upper else rows_ahead
            tail = tail + sp_whole - sp_tot
            whole = whole + sp_whole
            probed_start = unit * jnp.exp(totals - logdecay + sp_tot - spike_pair)
        tail = jnp.exp(tail)
        if queries is not None:
            weighted = jnp.exp(totals) * queries
            left.append(weighted)
            weighted_start = weighted
            if spike_pair is not None:
                weighted_start = queries * jnp.exp(totals + sp_tot)
        else:
            weighted_start = None
        strict = (row < col) if upper else (row > col)
        reach = (row <= col) if upper else (row >= col)
        right = jnp.concatenate([removal_in, key_in], axis=0)
        left = jnp.concatenate(left, axis=0)
        heads = []
        for number in range(2):
            own = first_head if number == 0 else jnp.logical_not(first_head)
            scores = low_dot_nt(jnp.where(own, left, 0.0), right)
            cols = slice(number * ATTEND_WIDTH, number * ATTEND_WIDTH + 1)
            if spike_pair is not None:
                shift = sp_tot[:, cols] - sp_row[number : number + 1, :]
                strict_fade = jnp.exp(jnp.minimum(shift - spike_pair[:, cols], 0.0))
                reach_fade = jnp.exp(jnp.minimum(shift, 0.0))
            else:
                strict_fade = reach_fade = 1.0
            system = jnp.where(strict, scores[:size, :size] * strict_fade, 0.0)
            inflow = jnp.where(strict, scores[:size, size:] * strict_fade, 0.0)
            if queries is not None:
                read_back = jnp.where(reach, scores[size:, :size] * reach_fade, 0.0)
                read_in = jnp.where(reach, scores[size:, size:] * reach_fade, 0.0)
            else:
                read_back = read_in = None
            heads.append((system, inflow, read_back, read_in))
        out.append(
            dict(
                heads=heads,
                probed_start=probed_start,
                weighted_start=weighted_start,
                keys_out=keys * tail,
                removal_out=removal * tail,
                final=jnp.exp(whole),
            )
        )
    return out


def pick(first_head, pair):
    return jnp.where(first_head, pair[0], pair[1])


def folded(block):
    kept = jnp.where(head_mask(PAIR), block, 0.0)
    return kept[:ATTEND_WIDTH] + kept[ATTEND_WIDTH:]


def unfolded(pair):
    return jnp.where(head_mask(PAIR), jnp.concatenate([pair, pair], axis=0), 0.0)


def chain_kernel(
    query_ref,
    key_ref,
    value_ref,
    low_ref,
    ctx_key_ref,
    ctx_value_ref,
    ctx_low_ref,
    raise_fading_ref,
    raise_step_ref,
    fading_ref,
    spike_ref,
    spike_row_ref,
    maps_ref,
    ctx_ref,
    reading_ref,
    inside_ref,
):
    lane = lax.broadcasted_iota(jnp.int32, (1, PAIR), 1)
    first_head = lane < ATTEND_WIDTH
    shared = (raise_fading_ref[...], raise_step_ref[...], fading_ref[...])
    keys = key_ref[...].astype(jnp.float32)
    values = value_ref[...].astype(jnp.float32)
    parts = token_features(keys, low_ref[...], *shared) + (keys, values)
    latent = chain_terms(
        parts, -spike_ref[...], -spike_row_ref[0], query_ref[...].astype(jnp.float32)
    )
    ctx_keys = ctx_key_ref[...].astype(jnp.float32)
    ctx_values = ctx_value_ref[...].astype(jnp.float32)
    ctx_parts = token_features(ctx_keys, ctx_low_ref[:, : low_ref.shape[1]], *shared) + (ctx_keys, ctx_values)
    context = chain_terms(ctx_parts, None, None, None)
    inverses = block_inverses([head[0] for terms in latent for head in terms["heads"]], None)
    ctx_inverses = block_inverses([head[0] for terms in context for head in terms["heads"]], None)
    inside = None
    for way in range(2):
        terms = latent[way]
        inverse = inverses[2 * way : 2 * way + 2]
        flow = pick(first_head, [low_dot(head[1], values) for head in terms["heads"]])
        joined = jnp.concatenate([terms["probed_start"], flow], axis=1)
        solved = [low_dot(one, joined) for one in inverse]
        on_state = pick(first_head, [one[:, :PAIR] for one in solved])
        alone = pick(first_head, [one[:, PAIR:] for one in solved])
        both = jnp.concatenate([on_state, alone], axis=1)
        back = [low_dot(head[2], both) for head in terms["heads"]]
        read = pick(first_head, [low_dot(head[3], values) for head in terms["heads"]])
        reading_ref[way] = (
            terms["weighted_start"] - pick(first_head, [one[:, :PAIR] for one in back])
        ).astype(reading_ref.dtype)
        part = read - pick(first_head, [one[:, PAIR:] for one in back])
        inside = part if inside is None else inside + part
        crossed = low_dot_tn(both, terms["removal_out"])
        eye = lax.broadcasted_iota(jnp.int32, (PAIR, PAIR), 0) == lax.broadcasted_iota(
            jnp.int32, (PAIR, PAIR), 1
        )
        factor = jnp.where(eye, terms["final"], 0.0) - crossed[:PAIR]
        offset = low_dot_tn(values, terms["keys_out"]) - crossed[PAIR:]
        maps_ref[way, 0, 0] = folded(factor).astype(maps_ref.dtype)
        maps_ref[way, 0, 1] = folded(offset).astype(maps_ref.dtype)
        ctx_terms = context[way]
        ctx_inverse = ctx_inverses[2 * way : 2 * way + 2]
        flow = pick(first_head, [low_dot(head[1], ctx_values) for head in ctx_terms["heads"]])
        alone = pick(first_head, [low_dot(one, flow) for one in ctx_inverse])
        ctx_ref[way, 0] = folded(
            low_dot_tn(ctx_values, ctx_terms["keys_out"])
            - low_dot_tn(alone, ctx_terms["removal_out"])
        )
    inside_ref[...] = inside


def chain_call(
    query, key, value, low, ctx_all, raise_fading, raise_step, fading, spike
):
    rows, width = key.shape
    ctx_rows = ctx_all.shape[0]
    pairs = width // PAIR
    rank = low.shape[1]
    spike_pair = jnp.repeat(spike, ATTEND_WIDTH, axis=1)
    spike_rows = jnp.transpose(spike).reshape(pairs, 2, rows)
    columns = lambda height: pl.BlockSpec((height, PAIR), lambda i: (0, i))
    entire = lambda height: pl.BlockSpec((height, rank), lambda i: (0, 0))
    return pl.pallas_call(
        chain_kernel,
        grid=(pairs,),
        in_specs=[
            columns(rows),
            columns(rows),
            columns(rows),
            entire(rows),
            columns(ctx_rows),
            pl.BlockSpec((ctx_rows, PAIR), lambda i: (0, pairs + i)),
            pl.BlockSpec((ctx_rows, PAIR), lambda i: (0, 2 * pairs)),
            columns(rank),
            columns(rank),
            columns(1),
            columns(rows),
            pl.BlockSpec((1, 2, rows), lambda i: (i, 0, 0)),
        ],
        out_specs=[
            pl.BlockSpec((2, 1, 2, ATTEND_WIDTH, PAIR), lambda i: (0, i, 0, 0, 0)),
            pl.BlockSpec((2, 1, ATTEND_WIDTH, PAIR), lambda i: (0, i, 0, 0)),
            pl.BlockSpec((2, rows, PAIR), lambda i: (0, 0, i)),
            columns(rows),
        ],
        out_shape=[
            jax.ShapeDtypeStruct((2, pairs, 2, ATTEND_WIDTH, PAIR), jnp.bfloat16),
            jax.ShapeDtypeStruct((2, pairs, ATTEND_WIDTH, PAIR), jnp.float32),
            jax.ShapeDtypeStruct((2, rows, width), jnp.bfloat16),
            jax.ShapeDtypeStruct((rows, width), jnp.float32),
        ],
        compiler_params=pltpu.CompilerParams(dimension_semantics=("arbitrary",)),
        cost_estimate=pl.CostEstimate(
            flops=pairs * 8 * 17 * 2 * PAIR**3, bytes_accessed=4 << 20, transcendentals=0
        ),
    )(
        query,
        key,
        value,
        low,
        ctx_all,
        ctx_all,
        ctx_all,
        raise_fading,
        raise_step,
        fading.reshape(1, width),
        spike_pair,
        spike_rows,
    )


MESH_ID = pl.DeviceIdType.MESH


def remote(source, target, send_sem, recv_sem, device):
    return pltpu.make_async_remote_copy(
        src_ref=source,
        dst_ref=target,
        send_sem=send_sem,
        recv_sem=recv_sem,
        device_id=device,
        device_id_type=MESH_ID,
    )


def greet(devices):
    barrier = pltpu.get_barrier_semaphore()
    for device in devices:
        pl.semaphore_signal(barrier, inc=1, device_id=device, device_id_type=MESH_ID)
    pl.semaphore_wait(barrier, len(devices))


def others(axis, count):
    own = lax.axis_index(axis)
    return [{axis: lax.rem(own + step, count)} for step in range(1, count)]


def front_kernel(
    sp_count,
    tp_count,
    active_ref,
    shift_ref,
    scale_ref,
    valve_ref,
    hidden_ref,
    prompt_ref,
    down_ref,
    rows_ref,
    ctx_ref,
    gates_ref,
    down_all_ref,
    partial_ref,
    vector_ref,
    down_send,
    down_recv,
    part_send,
    part_recv,
    vec_send,
    vec_recv,
    row_send,
    row_recv,
    mate_send,
    mate_recv,
):
    sp_own, tp_own = lax.axis_index("sp"), lax.axis_index("tp")
    sp_peers, tp_peers = others("sp", sp_count), others("tp", tp_count)
    greet(sp_peers + tp_peers)
    local = jnp.dot(active_ref[0], shift_ref[...], preferred_element_type=jnp.float32)
    local += jnp.dot(active_ref[1], scale_ref[...], preferred_element_type=jnp.float32)
    local += jnp.dot(active_ref[2], valve_ref[...], preferred_element_type=jnp.float32)
    partial_ref[0] = local[:8]
    part_copies = [
        remote(
            partial_ref.at[0],
            partial_ref.at[step + 1],
            part_send.at[step],
            part_recv.at[step],
            peer,
        )
        for step, peer in enumerate(sp_peers)
    ]
    for copy in part_copies:
        copy.start()
    down_copies = [
        remote(
            down_ref, down_all_ref.at[sp_own], down_send.at[step], down_recv.at[step], peer
        )
        for step, peer in enumerate(sp_peers)
    ]
    for copy in down_copies:
        copy.start()
    down_all_ref[sp_own] = down_ref[...]

    def statistics(ref):
        values = ref[...].astype(jnp.float32)
        centre = jnp.mean(values, -1, keepdims=True)
        spread = jnp.mean(jnp.square(values - centre), -1, keepdims=True)
        return centre, lax.rsqrt(spread + EPS_ROW)

    hidden_stats, prompt_stats = statistics(hidden_ref), statistics(prompt_ref)
    for copy in part_copies:
        copy.wait_recv()
    vector_ref[tp_own] = jnp.sum(partial_ref[...], axis=0)
    vec_copies = [
        remote(
            vector_ref.at[tp_own],
            vector_ref.at[tp_own],
            vec_send.at[step],
            vec_recv.at[step],
            peer,
        )
        for step, peer in enumerate(tp_peers)
    ]
    for copy in vec_copies:
        copy.start()
    for copy in vec_copies:
        copy.wait_recv()
    span = vector_ref.shape[2]

    def modulated(ref, stats, which, number):
        vector = vector_ref[number]
        values = ref[:, number * span : (number + 1) * span].astype(jnp.float32)
        normed = (values - stats[0]) * stats[1]
        changed = normed * (1.0 + vector[2 + which : 3 + which]) + vector[which : which + 1]
        return changed.astype(jnp.bfloat16)

    for number in range(tp_count):
        cols = slice(number * span, (number + 1) * span)
        rows_ref[tp_own, :, cols] = modulated(hidden_ref, hidden_stats, 0, number)
    chips = tp_count // 2
    chip, core = tp_own // 2, lax.rem(tp_own, 2)
    mate = {"tp": chip * 2 + 1 - core}
    height = rows_ref.shape[1]
    halves = 2 if height % 32 == 0 else 1
    part = height // halves
    spans = [pl.ds(half * part, part) for half in range(halves)]
    chip_copies = []
    for step in range(1, chips):
        target = {"tp": lax.rem(chip + step, chips) * 2 + core}
        for half, rows in enumerate(spans):
            slot = (step - 1) * halves + half
            block = rows_ref.at[tp_own, rows]
            chip_copies.append(
                remote(block, block, row_send.at[slot], row_recv.at[slot], target)
            )
    last = (chips - 1) * halves
    own_block = rows_ref.at[tp_own]
    mate_copies = [remote(own_block, own_block, mate_send.at[last], mate_recv.at[last], mate)]
    for copy in chip_copies + mate_copies:
        copy.start()
    for number in range(tp_count):
        cols = slice(number * span, (number + 1) * span)
        ctx_ref[:, cols] = modulated(prompt_ref, prompt_stats, 1, number)
        gates_ref[:, cols] = vector_ref[number, 4:5]
    for step in range(1, chips):
        source = lax.rem(chip + chips - step, chips) * 2 + core
        for half, rows in enumerate(spans):
            slot = (step - 1) * halves + half
            chip_copies[slot].wait_recv()
            block = rows_ref.at[source, rows]
            copy = remote(block, block, mate_send.at[slot], mate_recv.at[slot], mate)
            copy.start()
            mate_copies.append(copy)
    for copy in mate_copies + down_copies:
        copy.wait_recv()
    for copy in part_copies + down_copies + vec_copies + chip_copies + mate_copies:
        copy.wait_send()


VMEM_SPEC = pl.BlockSpec(memory_space=pltpu.VMEM)


def front_call(active, shift, scale, valve, hidden, prompt, down):
    sp_count, tp_count = lax.axis_size("sp"), lax.axis_size("tp")
    width = hidden.shape[1]
    dma = pltpu.SemaphoreType.DMA
    return pl.pallas_call(
        functools.partial(front_kernel, sp_count, tp_count),
        in_specs=[VMEM_SPEC] * 7,
        out_specs=[VMEM_SPEC] * 4,
        out_shape=[
            jax.ShapeDtypeStruct((tp_count,) + hidden.shape, jnp.bfloat16),
            jax.ShapeDtypeStruct(prompt.shape, jnp.bfloat16),
            jax.ShapeDtypeStruct((1, width), jnp.float32),
            jax.ShapeDtypeStruct((sp_count,) + down.shape, jnp.bfloat16),
        ],
        scratch_shapes=[
            pltpu.VMEM((sp_count, 8, shift.shape[1]), jnp.float32),
            pltpu.VMEM((tp_count, 8, shift.shape[1]), jnp.float32),
        ]
        + [dma((sp_count,))] * 4
        + [dma((tp_count,))] * 6,
        compiler_params=pltpu.CompilerParams(collective_id=0, has_side_effects=True),
        cost_estimate=pl.CostEstimate(
            flops=1 << 20, bytes_accessed=60 << 20, transcendentals=0
        ),
    )(active, shift, scale, valve, hidden, prompt, down)


def spread_kernel(count, own_ref, all_ref, send, recv):
    own = lax.axis_index("sp")
    peers = others("sp", count)
    greet(peers)
    copies = [
        remote(own_ref, all_ref.at[own], send.at[step], recv.at[step], peer)
        for step, peer in enumerate(peers)
    ]
    for copy in copies:
        copy.start()
    all_ref[own] = own_ref[...]
    for copy in copies:
        copy.wait()


def spread_call(block):
    count = lax.axis_size("sp")
    dma = pltpu.SemaphoreType.DMA
    return pl.pallas_call(
        functools.partial(spread_kernel, count),
        in_specs=[VMEM_SPEC],
        out_specs=VMEM_SPEC,
        out_shape=jax.ShapeDtypeStruct((count,) + block.shape, block.dtype),
        scratch_shapes=[dma((count,)), dma((count,))],
        compiler_params=pltpu.CompilerParams(collective_id=1, has_side_effects=True),
        cost_estimate=pl.CostEstimate(
            flops=1 << 20, bytes_accessed=20 << 20, transcendentals=0
        ),
    )(block)


def read_kernel(
    count,
    maps_ref,
    ctx_ref,
    reading_ref,
    inside_ref,
    gains_ref,
    normed_ref,
    slots_ref,
    state_ref,
    send,
    recv,
):
    own = lax.axis_index("sp")
    pairs = maps_ref.shape[1]
    greet(others("sp", count))

    def transfer(way, step):
        target = own + step if way == 0 else own - step
        target = jnp.clip(target, 0, count - 1)
        return remote(
            maps_ref.at[way],
            slots_ref.at[way, step - 1],
            send.at[way, step - 1],
            recv.at[way, step - 1],
            {"sp": target},
        )

    def sending(way, step):
        return own + step < count if way == 0 else own >= step

    def receiving(way, step):
        return own >= step if way == 0 else own + step < count

    for step in range(count - 1, 0, -1):
        for way in range(2):

            @pl.when(sending(way, step))
            def _():
                transfer(way, step).start()

    for way in range(2):
        for pair in range(pairs):
            state_ref[way, pair] = unfolded(ctx_ref[way, pair])
    for step in range(count - 1, 0, -1):
        for way in range(2):

            @pl.when(receiving(way, step))
            def _():
                transfer(way, step).wait_recv()
                for pair in range(pairs):
                    factor = unfolded(slots_ref[way, step - 1, pair, 0].astype(jnp.float32))
                    offset = unfolded(slots_ref[way, step - 1, pair, 1].astype(jnp.float32))
                    state_ref[way, pair] = low_dot(state_ref[way, pair], factor) + offset

    same_head = head_mask(PAIR).astype(jnp.float32) * (1.0 / ATTEND_WIDTH)
    for pair in range(pairs):
        cols = slice(pair * PAIR, (pair + 1) * PAIR)
        combined = (
            inside_ref[:, cols]
            + low_dot_nt(reading_ref[0, :, cols], state_ref[0, pair])
            + low_dot_nt(reading_ref[1, :, cols], state_ref[1, pair])
        )
        centred = combined - exact_dot(combined, same_head)
        spread = exact_dot(centred * centred, same_head)
        normed = centred * lax.rsqrt(spread + EPS_HEAD) * gains_ref[:, cols]
        normed_ref[:, cols] = normed.astype(normed_ref.dtype)
    for step in range(count - 1, 0, -1):
        for way in range(2):

            @pl.when(sending(way, step))
            def _():
                transfer(way, step).wait_send()


def read_call(maps, ctx, reading, inside, gains):
    rows, width = inside.shape
    count = lax.axis_size("sp")
    dma = pltpu.SemaphoreType.DMA
    return pl.pallas_call(
        functools.partial(read_kernel, count),
        in_specs=[VMEM_SPEC] * 5,
        out_specs=VMEM_SPEC,
        out_shape=jax.ShapeDtypeStruct((rows, width), jnp.bfloat16),
        scratch_shapes=[
            pltpu.VMEM((2, count - 1) + maps.shape[1:], jnp.bfloat16),
            pltpu.VMEM((2, maps.shape[1], PAIR, PAIR), jnp.float32),
            dma((2, count - 1)),
            dma((2, count - 1)),
        ],
        compiler_params=pltpu.CompilerParams(collective_id=2, has_side_effects=True),
        cost_estimate=pl.CostEstimate(
            flops=8 * 4 * 2 * PAIR**3, bytes_accessed=40 << 20, transcendentals=0
        ),
    )(maps, ctx, reading, inside, gains.reshape(1, width))


def emit_kernel(
    tp_count,
    normed_ref,
    weight_ref,
    hidden_ref,
    gates_ref,
    out_ref,
    product_ref,
    mate_ref,
    chip_ref,
    land_ref,
    mate_send,
    mate_recv,
    chip_send,
    chip_recv,
):
    tp_own = lax.axis_index("tp")
    chips = tp_count // 2
    chip, core = tp_own // 2, lax.rem(tp_own, 2)
    mate = {"tp": chip * 2 + 1 - core}
    targets = [{"tp": lax.rem(chip + step, chips) * 2 + core} for step in range(1, chips)]
    greet([mate] + targets)
    pieces = product_ref.shape[0]
    span = product_ref.shape[4]
    height = out_ref.shape[0]
    shape = (chips, 2, height, span)
    mate_copies = []
    for piece in range(pieces):
        cols = slice(piece * span, (piece + 1) * span)
        block = jnp.dot(
            normed_ref[...], weight_ref[:, cols], preferred_element_type=jnp.float32
        ).astype(jnp.bfloat16)
        for place in range(chips):
            for side in range(2):
                first = (place * 2 + side) * height
                product_ref[piece, side, place] = block[first : first + height]
        copy = remote(
            product_ref.at[piece, 1 - core],
            mate_ref.at[piece],
            mate_send.at[piece],
            mate_recv.at[piece],
            mate,
        )
        copy.start()
        mate_copies.append(copy)
    chip_copies = []
    for piece in range(pieces):
        mate_copies[piece].wait_recv()
        summed = product_ref[piece, core].astype(jnp.float32) + mate_ref[piece].astype(
            jnp.float32
        )
        chip_ref[piece] = summed.astype(jnp.bfloat16)
        for step, target in enumerate(targets):
            copy = remote(
                chip_ref.at[piece, lax.rem(chip + step + 1, chips)],
                land_ref.at[piece, step],
                chip_send.at[piece, step],
                chip_recv.at[piece, step],
                target,
            )
            copy.start()
            chip_copies.append(copy)
    for piece in range(pieces):
        cols = slice(piece * span, (piece + 1) * span)
        mixed = product_ref[piece, core, chip].astype(jnp.float32) + mate_ref[
            piece, chip
        ].astype(jnp.float32)
        for step in range(chips - 1):
            chip_copies[piece * (chips - 1) + step].wait_recv()
            mixed += land_ref[piece, step].astype(jnp.float32)
        out_ref[:, cols] = (
            hidden_ref[:, cols].astype(jnp.float32) + gates_ref[:, cols] * mixed
        ).astype(out_ref.dtype)
    for copy in mate_copies + chip_copies:
        copy.wait_send()


def emit_call(normed, weight, hidden, gates):
    tp_count = lax.axis_size("tp")
    chips = tp_count // 2
    height, width = hidden.shape
    pieces = math.gcd(4, width // PAIR)
    span = width // pieces
    dma = pltpu.SemaphoreType.DMA
    vmem = lambda *shape: pltpu.VMEM(shape, jnp.bfloat16)
    return pl.pallas_call(
        functools.partial(emit_kernel, tp_count),
        in_specs=[VMEM_SPEC] * 4,
        out_specs=VMEM_SPEC,
        out_shape=jax.ShapeDtypeStruct(hidden.shape, jnp.bfloat16),
        scratch_shapes=[
            vmem(pieces, 2, chips, height, span),
            vmem(pieces, chips, height, span),
            vmem(pieces, chips, height, span),
            vmem(pieces, chips - 1, height, span),
            dma((pieces,)),
            dma((pieces,)),
            dma((pieces, chips - 1)),
            dma((pieces, chips - 1)),
        ],
        compiler_params=pltpu.CompilerParams(collective_id=3, has_side_effects=True),
    )(normed, weight, hidden, gates)


def body(
    hidden_items,
    sample_cond,
    prompt_items,
    prompt_cond,
    adjust_shifting,
    adjust_stretch,
    skip_valve,
    receiver_matrix,
    address_matrix,
    payload_matrix,
    joint_lower_projector,
    fading_raise_matrix,
    step_raise_matrix,
    feature_fading,
    spike_logfade,
    group_standard_factor,
    emit_matrix,
):
    span_rows = adjust_shifting.shape[0]
    conditions = jnp.stack([sample_cond, prompt_cond])
    activated = jax.nn.silu(conditions.astype(jnp.float32)).astype(jnp.bfloat16)
    own_cols = lax.dynamic_slice_in_dim(activated, lax.axis_index("sp") * span_rows, span_rows, 1)
    active = jnp.stack(
        [
            jnp.pad(own_cols, ((0, 14), (0, 0))),
            jnp.pad(own_cols, ((2, 12), (0, 0))),
            jnp.pad(own_cols[:1], ((4, 11), (0, 0))),
        ]
    )
    half = joint_lower_projector.shape[0] // 2
    down_own = jnp.concatenate(
        [joint_lower_projector[:half], joint_lower_projector[half:]], axis=1
    )
    out_weight = lax.all_gather(emit_matrix, "sp", axis=1, tiled=True)
    features, ctx_mod, gates, down_all = front_call(
        active,
        adjust_shifting,
        adjust_stretch,
        skip_valve,
        hidden_items,
        prompt_items,
        down_own,
    )
    features = features.reshape(-1, hidden_items.shape[1])
    rank = joint_lower_projector.shape[1]
    down_weight = jnp.stack([down_all[:, :, :rank], down_all[:, :, rank:]], axis=1)
    down_weight = down_weight.reshape(-1, rank)
    ctx_key = stored(product(ctx_mod, address_matrix))
    ctx_value = stored(product(ctx_mod, payload_matrix))
    ctx_low = stored(product(ctx_mod, down_weight))
    ctx_joined = jnp.concatenate(
        [ctx_key, ctx_value, jnp.pad(ctx_low, ((0, 0), (0, PAIR - rank)))], axis=1
    )
    ctx_all = spread_call(ctx_joined).reshape(-1, ctx_joined.shape[1])
    maps, ctx_state, reading, inside = chain_call(
        stored(product(features, receiver_matrix)),
        stored(product(features, address_matrix)),
        stored(product(features, payload_matrix)),
        stored(product(features, down_weight)),
        ctx_all,
        fading_raise_matrix,
        step_raise_matrix,
        feature_fading,
        spike_logfade,
    )
    normed = read_call(maps, ctx_state, reading, inside, group_standard_factor)
    return emit_call(normed, out_weight, hidden_items, gates)


def solution(mesh):
    placed = (
        P(("grp", "sp", "tp"), None),
        P("grp"),
        P(("grp", "sp"), None),
        P(),
        P("sp", "tp"),
        P("sp", "tp"),
        P("sp", "tp"),
        P(None, "tp"),
        P(None, "tp"),
        P(None, "tp"),
        P("sp", None),
        P(None, "tp"),
        P(None, "tp"),
        P("tp"),
        P(("grp", "sp"), "tp"),
        P("tp"),
        P("tp", "sp"),
    )
    return jax.shard_map(
        body, mesh=mesh, in_specs=placed, out_specs=P(("grp", "sp", "tp"), None), check_vma=False
    )
```

```python
import functools

import jax
import jax.numpy as jnp
from jax import lax
from jax.experimental import pallas as pl
from jax.experimental.pallas import tpu as pltpu
from jax.sharding import PartitionSpec as P

ATTEND_WIDTH = 64
PAIR = 2 * ATTEND_WIDTH

EXACT_MODE = lax.Precision.HIGHEST
EPS_ROW = 1e-05
EPS_HEAD = 0.00064
EPS_KEY = 1e-06
rate_shift = 5.0


def stored(value):
    return lax.optimization_barrier(value.astype(jnp.bfloat16))


def product(left, right):
    return jnp.dot(left, right, preferred_element_type=jnp.float32)


def modulate(rows, shifts, scales):
    values = rows.astype(jnp.float32)
    centre = jnp.mean(values, -1, keepdims=True)
    spread = jnp.mean(jnp.square(values - centre), -1, keepdims=True)
    normed = (values - centre) * lax.rsqrt(spread + EPS_ROW)
    return (normed * (1.0 + scales) + shifts).astype(jnp.bfloat16)


def low_dot(left, right):
    return jnp.dot(
        left.astype(jnp.bfloat16), right.astype(jnp.bfloat16), preferred_element_type=jnp.float32
    )


def low_dot_nt(left, right):
    return lax.dot_general(
        left.astype(jnp.bfloat16),
        right.astype(jnp.bfloat16),
        (((1,), (1,)), ((), ())),
        preferred_element_type=jnp.float32,
    )


def low_dot_tn(left, right):
    return lax.dot_general(
        left.astype(jnp.bfloat16),
        right.astype(jnp.bfloat16),
        (((0,), (0,)), ((), ())),
        preferred_element_type=jnp.float32,
    )


def exact_dot(left, right):
    return jnp.dot(left, right, precision=EXACT_MODE, preferred_element_type=jnp.float32)


def head_mask(size):
    row = lax.broadcasted_iota(jnp.int32, (size, size), 0)
    col = lax.broadcasted_iota(jnp.int32, (size, size), 1)
    return (row // ATTEND_WIDTH) == (col // ATTEND_WIDTH)


def token_features(keys, lows, raise_fading, raise_step, fading):
    squashed = jnp.tanh(lows.astype(jnp.float32)).astype(jnp.bfloat16)
    logdecay = -fading * jax.nn.sigmoid(product(squashed, raise_fading))
    learned = jax.nn.sigmoid(product(squashed, raise_step) - rate_shift)
    same_head = head_mask(PAIR).astype(jnp.float32)
    unit = keys * lax.rsqrt(exact_dot(keys * keys, same_head) + EPS_KEY)
    return unit, unit * learned, logdecay


def block_inverses(systems, uppers):
    size = systems[0].shape[0]
    row = lax.broadcasted_iota(jnp.int32, (size, size), 0)
    col = lax.broadcasted_iota(jnp.int32, (size, size), 1)
    eye = (row == col).astype(jnp.float32)
    inverses = None
    width = 1
    while width < size:
        merged = (row // (2 * width) == col // (2 * width)) & (row // width != col // width)
        pieces = [jnp.where(merged, system, 0.0) for system in systems]
        if inverses is None:
            inverses = [eye - piece for piece in pieces]
        else:
            firsts = [low_dot(inverse, piece) for inverse, piece in zip(inverses, pieces)]
            inverses = [
                inverse - low_dot(first, inverse) for first, inverse in zip(firsts, inverses)
            ]
        width *= 2
    return inverses


def chain_terms(parts, spike_pair, spike_rows, queries):
    unit, removal, logdecay, keys, values = parts
    size = keys.shape[0]
    row = lax.broadcasted_iota(jnp.int32, (size, size), 0)
    col = lax.broadcasted_iota(jnp.int32, (size, size), 1)
    lane = lax.broadcasted_iota(jnp.int32, (1, PAIR), 1)
    first_head = lane < ATTEND_WIDTH
    upto = (row >= col).astype(jnp.float32)
    ahead = exact_dot(upto, logdecay)
    behind = ahead[-1:, :] - ahead + logdecay
    if spike_pair is not None:
        spike_ahead = exact_dot(upto, spike_pair)
        spike_behind = spike_ahead[-1:, :] - spike_ahead + spike_pair
        rows_ahead = exact_dot(spike_rows, (row <= col).astype(jnp.float32))
        rows_behind = exact_dot(spike_rows, (row >= col).astype(jnp.float32))
    out = []
    for upper in (False, True):
        totals = behind if upper else ahead
        whole = totals[:1, :] if upper else totals[-1:, :]
        inverse = jnp.exp(-totals)
        exclusive = jnp.exp(totals - logdecay)
        probed = exclusive * unit
        key_in = keys * inverse
        removal_in = removal * inverse
        left = [probed]
        tail = whole - totals
        probed_start = probed
        if spike_pair is not None:
            sp_tot = spike_behind if upper else spike_ahead
            sp_whole = sp_tot[:1, :] if upper else sp_tot[-1:, :]
            sp_row = rows_behind if upper else rows_ahead
            tail = tail + sp_whole - sp_tot
            whole = whole + sp_whole
            probed_start = unit * jnp.exp(totals - logdecay + sp_tot - spike_pair)
        tail = jnp.exp(tail)
        if queries is not None:
            weighted = jnp.exp(totals) * queries
            left.append(weighted)
            weighted_start = weighted
            if spike_pair is not None:
                weighted_start = queries * jnp.exp(totals + sp_tot)
        else:
            weighted_start = None
        strict = (row < col) if upper else (row > col)
        reach = (row <= col) if upper else (row >= col)
        right = jnp.concatenate([removal_in, key_in], axis=0)
        left = jnp.concatenate(left, axis=0)
        heads = []
        for number in range(2):
            own = first_head if number == 0 else jnp.logical_not(first_head)
            scores = low_dot_nt(jnp.where(own, left, 0.0), right)
            cols = slice(number * ATTEND_WIDTH, number * ATTEND_WIDTH + 1)
            if spike_pair is not None:
                shift = sp_tot[:, cols] - sp_row[number : number + 1, :]
                strict_fade = jnp.exp(jnp.minimum(shift - spike_pair[:, cols], 0.0))
                reach_fade = jnp.exp(jnp.minimum(shift, 0.0))
            else:
                strict_fade = reach_fade = 1.0
            system = jnp.where(strict, scores[:size, :size] * strict_fade, 0.0)
            inflow = jnp.where(strict, scores[:size, size:] * strict_fade, 0.0)
            if queries is not None:
                read_back = jnp.where(reach, scores[size:, :size] * reach_fade, 0.0)
                read_in = jnp.where(reach, scores[size:, size:] * reach_fade, 0.0)
            else:
                read_back = read_in = None
            heads.append((system, inflow, read_back, read_in))
        out.append(
            dict(
                heads=heads,
                probed_start=probed_start,
                weighted_start=weighted_start,
                keys_out=keys * tail,
                removal_out=removal * tail,
                final=jnp.exp(whole),
            )
        )
    return out


def pick(first_head, pair):
    return jnp.where(first_head, pair[0], pair[1])


def folded(block):
    kept = jnp.where(head_mask(PAIR), block, 0.0)
    return kept[:ATTEND_WIDTH] + kept[ATTEND_WIDTH:]


def unfolded(pair):
    return jnp.where(head_mask(PAIR), jnp.concatenate([pair, pair], axis=0), 0.0)


def chain_kernel(
    query_ref,
    key_ref,
    value_ref,
    low_ref,
    ctx_key_ref,
    ctx_value_ref,
    ctx_low_ref,
    raise_fading_ref,
    raise_step_ref,
    fading_ref,
    spike_ref,
    spike_row_ref,
    maps_ref,
    ctx_ref,
    reading_ref,
    inside_ref,
):
    lane = lax.broadcasted_iota(jnp.int32, (1, PAIR), 1)
    first_head = lane < ATTEND_WIDTH
    shared = (raise_fading_ref[...], raise_step_ref[...], fading_ref[...])
    keys = key_ref[...].astype(jnp.float32)
    values = value_ref[...].astype(jnp.float32)
    parts = token_features(keys, low_ref[...], *shared) + (keys, values)
    latent = chain_terms(
        parts, -spike_ref[...], -spike_row_ref[0], query_ref[...].astype(jnp.float32)
    )
    ctx_keys = ctx_key_ref[...].astype(jnp.float32)
    ctx_values = ctx_value_ref[...].astype(jnp.float32)
    ctx_parts = token_features(ctx_keys, ctx_low_ref[:, : low_ref.shape[1]], *shared) + (ctx_keys, ctx_values)
    context = chain_terms(ctx_parts, None, None, None)
    inverses = block_inverses([head[0] for terms in latent for head in terms["heads"]], None)
    ctx_inverses = block_inverses([head[0] for terms in context for head in terms["heads"]], None)
    inside = None
    for way in range(2):
        terms = latent[way]
        inverse = inverses[2 * way : 2 * way + 2]
        flow = pick(first_head, [low_dot(head[1], values) for head in terms["heads"]])
        joined = jnp.concatenate([terms["probed_start"], flow], axis=1)
        solved = [low_dot(one, joined) for one in inverse]
        on_state = pick(first_head, [one[:, :PAIR] for one in solved])
        alone = pick(first_head, [one[:, PAIR:] for one in solved])
        both = jnp.concatenate([on_state, alone], axis=1)
        back = [low_dot(head[2], both) for head in terms["heads"]]
        read = pick(first_head, [low_dot(head[3], values) for head in terms["heads"]])
        reading_ref[way] = (
            terms["weighted_start"] - pick(first_head, [one[:, :PAIR] for one in back])
        ).astype(reading_ref.dtype)
        part = read - pick(first_head, [one[:, PAIR:] for one in back])
        inside = part if inside is None else inside + part
        crossed = low_dot_tn(both, terms["removal_out"])
        eye = lax.broadcasted_iota(jnp.int32, (PAIR, PAIR), 0) == lax.broadcasted_iota(
            jnp.int32, (PAIR, PAIR), 1
        )
        factor = jnp.where(eye, terms["final"], 0.0) - crossed[:PAIR]
        offset = low_dot_tn(values, terms["keys_out"]) - crossed[PAIR:]
        maps_ref[way, 0, 0] = folded(factor).astype(maps_ref.dtype)
        maps_ref[way, 0, 1] = folded(offset).astype(maps_ref.dtype)
        ctx_terms = context[way]
        ctx_inverse = ctx_inverses[2 * way : 2 * way + 2]
        flow = pick(first_head, [low_dot(head[1], ctx_values) for head in ctx_terms["heads"]])
        alone = pick(first_head, [low_dot(one, flow) for one in ctx_inverse])
        ctx_ref[way, 0] = folded(
            low_dot_tn(ctx_values, ctx_terms["keys_out"])
            - low_dot_tn(alone, ctx_terms["removal_out"])
        )
    inside_ref[...] = inside


def chain_call(
    query, key, value, low, ctx_all, raise_fading, raise_step, fading, spike
):
    rows, width = key.shape
    ctx_rows = ctx_all.shape[0]
    pairs = width // PAIR
    rank = low.shape[1]
    spike_pair = jnp.repeat(spike, ATTEND_WIDTH, axis=1)
    spike_rows = jnp.transpose(spike).reshape(pairs, 2, rows)
    columns = lambda height: pl.BlockSpec((height, PAIR), lambda i: (0, i))
    entire = lambda height: pl.BlockSpec((height, rank), lambda i: (0, 0))
    return pl.pallas_call(
        chain_kernel,
        grid=(pairs,),
        in_specs=[
            columns(rows),
            columns(rows),
            columns(rows),
            entire(rows),
            columns(ctx_rows),
            pl.BlockSpec((ctx_rows, PAIR), lambda i: (0, pairs + i)),
            pl.BlockSpec((ctx_rows, PAIR), lambda i: (0, 2 * pairs)),
            columns(rank),
            columns(rank),
            columns(1),
            columns(rows),
            pl.BlockSpec((1, 2, rows), lambda i: (i, 0, 0)),
        ],
        out_specs=[
            pl.BlockSpec((2, 1, 2, ATTEND_WIDTH, PAIR), lambda i: (0, i, 0, 0, 0)),
            pl.BlockSpec((2, 1, ATTEND_WIDTH, PAIR), lambda i: (0, i, 0, 0)),
            pl.BlockSpec((2, rows, PAIR), lambda i: (0, 0, i)),
            columns(rows),
        ],
        out_shape=[
            jax.ShapeDtypeStruct((2, pairs, 2, ATTEND_WIDTH, PAIR), jnp.bfloat16),
            jax.ShapeDtypeStruct((2, pairs, ATTEND_WIDTH, PAIR), jnp.float32),
            jax.ShapeDtypeStruct((2, rows, width), jnp.bfloat16),
            jax.ShapeDtypeStruct((rows, width), jnp.float32),
        ],
        compiler_params=pltpu.CompilerParams(dimension_semantics=("arbitrary",)),
        cost_estimate=pl.CostEstimate(
            flops=pairs * 8 * 17 * 2 * PAIR**3, bytes_accessed=4 << 20, transcendentals=0
        ),
    )(
        query,
        key,
        value,
        low,
        ctx_all,
        ctx_all,
        ctx_all,
        raise_fading,
        raise_step,
        fading.reshape(1, width),
        spike_pair,
        spike_rows,
    )


MESH_ID = pl.DeviceIdType.MESH


def remote(source, target, send_sem, recv_sem, device):
    return pltpu.make_async_remote_copy(
        src_ref=source,
        dst_ref=target,
        send_sem=send_sem,
        recv_sem=recv_sem,
        device_id=device,
        device_id_type=MESH_ID,
    )


def greet(devices):
    barrier = pltpu.get_barrier_semaphore()
    for device in devices:
        pl.semaphore_signal(barrier, inc=1, device_id=device, device_id_type=MESH_ID)
    pl.semaphore_wait(barrier, len(devices))


def others(axis, count):
    own = lax.axis_index(axis)
    return [{axis: lax.rem(own + step, count)} for step in range(1, count)]


def front_kernel(
    sp_count,
    tp_count,
    active_ref,
    shift_ref,
    scale_ref,
    valve_ref,
    hidden_ref,
    prompt_ref,
    down_ref,
    rows_ref,
    ctx_ref,
    gates_ref,
    down_all_ref,
    partial_ref,
    vector_ref,
    down_send,
    down_recv,
    part_send,
    part_recv,
    vec_send,
    vec_recv,
    row_send,
    row_recv,
    mate_send,
    mate_recv,
):
    sp_own, tp_own = lax.axis_index("sp"), lax.axis_index("tp")
    sp_peers, tp_peers = others("sp", sp_count), others("tp", tp_count)
    greet(sp_peers + tp_peers)
    local = jnp.dot(active_ref[0], shift_ref[...], preferred_element_type=jnp.float32)
    local += jnp.dot(active_ref[1], scale_ref[...], preferred_element_type=jnp.float32)
    local += jnp.dot(active_ref[2], valve_ref[...], preferred_element_type=jnp.float32)
    partial_ref[0] = local[:8]
    part_copies = [
        remote(
            partial_ref.at[0],
            partial_ref.at[step + 1],
            part_send.at[step],
            part_recv.at[step],
            peer,
        )
        for step, peer in enumerate(sp_peers)
    ]
    for copy in part_copies:
        copy.start()
    down_copies = [
        remote(
            down_ref, down_all_ref.at[sp_own], down_send.at[step], down_recv.at[step], peer
        )
        for step, peer in enumerate(sp_peers)
    ]
    for copy in down_copies:
        copy.start()
    down_all_ref[sp_own] = down_ref[...]

    def statistics(ref):
        values = ref[...].astype(jnp.float32)
        centre = jnp.mean(values, -1, keepdims=True)
        spread = jnp.mean(jnp.square(values - centre), -1, keepdims=True)
        return centre, lax.rsqrt(spread + EPS_ROW)

    hidden_stats, prompt_stats = statistics(hidden_ref), statistics(prompt_ref)
    for copy in part_copies:
        copy.wait_recv()
    vector_ref[tp_own] = jnp.sum(partial_ref[...], axis=0)
    vec_copies = [
        remote(
            vector_ref.at[tp_own],
            vector_ref.at[tp_own],
            vec_send.at[step],
            vec_recv.at[step],
            peer,
        )
        for step, peer in enumerate(tp_peers)
    ]
    for copy in vec_copies:
        copy.start()
    for copy in vec_copies:
        copy.wait_recv()
    span = vector_ref.shape[2]

    def modulated(ref, stats, which, number):
        vector = vector_ref[number]
        values = ref[:, number * span : (number + 1) * span].astype(jnp.float32)
        normed = (values - stats[0]) * stats[1]
        changed = normed * (1.0 + vector[2 + which : 3 + which]) + vector[which : which + 1]
        return changed.astype(jnp.bfloat16)

    for number in range(tp_count):
        cols = slice(number * span, (number + 1) * span)
        rows_ref[tp_own, :, cols] = modulated(hidden_ref, hidden_stats, 0, number)
    chips = tp_count // 2
    chip, core = tp_own // 2, lax.rem(tp_own, 2)
    mate = {"tp": chip * 2 + 1 - core}
    height = rows_ref.shape[1]
    halves = 2 if height % 32 == 0 else 1
    part = height // halves
    spans = [pl.ds(half * part, part) for half in range(halves)]
    chip_copies = []
    for step in range(1, chips):
        target = {"tp": lax.rem(chip + step, chips) * 2 + core}
        for half, rows in enumerate(spans):
            slot = (step - 1) * halves + half
            block = rows_ref.at[tp_own, rows]
            chip_copies.append(
                remote(block, block, row_send.at[slot], row_recv.at[slot], target)
            )
    last = (chips - 1) * halves
    own_block = rows_ref.at[tp_own]
    mate_copies = [remote(own_block, own_block, mate_send.at[last], mate_recv.at[last], mate)]
    for copy in chip_copies + mate_copies:
        copy.start()
    for number in range(tp_count):
        cols = slice(number * span, (number + 1) * span)
        ctx_ref[:, cols] = modulated(prompt_ref, prompt_stats, 1, number)
        gates_ref[:, cols] = vector_ref[number, 4:5]
    for step in range(1, chips):
        source = lax.rem(chip + chips - step, chips) * 2 + core
        for half, rows in enumerate(spans):
            slot = (step - 1) * halves + half
            chip_copies[slot].wait_recv()
            block = rows_ref.at[source, rows]
            copy = remote(block, block, mate_send.at[slot], mate_recv.at[slot], mate)
            copy.start()
            mate_copies.append(copy)
    for copy in mate_copies + down_copies:
        copy.wait_recv()
    for copy in part_copies + down_copies + vec_copies + chip_copies + mate_copies:
        copy.wait_send()


VMEM_SPEC = pl.BlockSpec(memory_space=pltpu.VMEM)


def front_call(active, shift, scale, valve, hidden, prompt, down):
    sp_count, tp_count = lax.axis_size("sp"), lax.axis_size("tp")
    width = hidden.shape[1]
    dma = pltpu.SemaphoreType.DMA
    return pl.pallas_call(
        functools.partial(front_kernel, sp_count, tp_count),
        in_specs=[VMEM_SPEC] * 7,
        out_specs=[VMEM_SPEC] * 4,
        out_shape=[
            jax.ShapeDtypeStruct((tp_count,) + hidden.shape, jnp.bfloat16),
            jax.ShapeDtypeStruct(prompt.shape, jnp.bfloat16),
            jax.ShapeDtypeStruct((1, width), jnp.float32),
            jax.ShapeDtypeStruct((sp_count,) + down.shape, jnp.bfloat16),
        ],
        scratch_shapes=[
            pltpu.VMEM((sp_count, 8, shift.shape[1]), jnp.float32),
            pltpu.VMEM((tp_count, 8, shift.shape[1]), jnp.float32),
        ]
        + [dma((sp_count,))] * 4
        + [dma((tp_count,))] * 6,
        compiler_params=pltpu.CompilerParams(collective_id=0, has_side_effects=True),
        cost_estimate=pl.CostEstimate(
            flops=1 << 20, bytes_accessed=60 << 20, transcendentals=0
        ),
    )(active, shift, scale, valve, hidden, prompt, down)


def spread_kernel(count, own_ref, all_ref, send, recv):
    own = lax.axis_index("sp")
    peers = others("sp", count)
    greet(peers)
    copies = [
        remote(own_ref, all_ref.at[own], send.at[step], recv.at[step], peer)
        for step, peer in enumerate(peers)
    ]
    for copy in copies:
        copy.start()
    all_ref[own] = own_ref[...]
    for copy in copies:
        copy.wait()


def spread_call(block, collective_id):
    count = lax.axis_size("sp")
    dma = pltpu.SemaphoreType.DMA
    return pl.pallas_call(
        functools.partial(spread_kernel, count),
        in_specs=[VMEM_SPEC],
        out_specs=VMEM_SPEC,
        out_shape=jax.ShapeDtypeStruct((count,) + block.shape, block.dtype),
        scratch_shapes=[dma((count,)), dma((count,))],
        compiler_params=pltpu.CompilerParams(collective_id=collective_id, has_side_effects=True),
        cost_estimate=pl.CostEstimate(
            flops=1 << 20, bytes_accessed=20 << 20, transcendentals=0
        ),
    )(block)


def read_kernel(
    count,
    maps_ref,
    ctx_ref,
    reading_ref,
    inside_ref,
    gains_ref,
    normed_ref,
    slots_ref,
    state_ref,
    send,
    recv,
):
    own = lax.axis_index("sp")
    pairs = maps_ref.shape[1]
    greet(others("sp", count))

    def transfer(way, step):
        target = own + step if way == 0 else own - step
        target = jnp.clip(target, 0, count - 1)
        return remote(
            maps_ref.at[way],
            slots_ref.at[way, step - 1],
            send.at[way, step - 1],
            recv.at[way, step - 1],
            {"sp": target},
        )

    def sending(way, step):
        return own + step < count if way == 0 else own >= step

    def receiving(way, step):
        return own >= step if way == 0 else own + step < count

    for step in range(count - 1, 0, -1):
        for way in range(2):

            @pl.when(sending(way, step))
            def _():
                transfer(way, step).start()

    for way in range(2):
        for pair in range(pairs):
            state_ref[way, pair] = unfolded(ctx_ref[way, pair])
    for step in range(count - 1, 0, -1):
        for way in range(2):

            @pl.when(receiving(way, step))
            def _():
                transfer(way, step).wait_recv()
                for pair in range(pairs):
                    factor = unfolded(slots_ref[way, step - 1, pair, 0].astype(jnp.float32))
                    offset = unfolded(slots_ref[way, step - 1, pair, 1].astype(jnp.float32))
                    state_ref[way, pair] = low_dot(state_ref[way, pair], factor) + offset

    same_head = head_mask(PAIR).astype(jnp.float32) * (1.0 / ATTEND_WIDTH)
    for pair in range(pairs):
        cols = slice(pair * PAIR, (pair + 1) * PAIR)
        combined = (
            inside_ref[:, cols]
            + low_dot_nt(reading_ref[0, :, cols], state_ref[0, pair])
            + low_dot_nt(reading_ref[1, :, cols], state_ref[1, pair])
        )
        centred = combined - exact_dot(combined, same_head)
        spread = exact_dot(centred * centred, same_head)
        normed = centred * lax.rsqrt(spread + EPS_HEAD) * gains_ref[:, cols]
        normed_ref[:, cols] = normed.astype(normed_ref.dtype)
    for step in range(count - 1, 0, -1):
        for way in range(2):

            @pl.when(sending(way, step))
            def _():
                transfer(way, step).wait_send()


def read_call(maps, ctx, reading, inside, gains):
    rows, width = inside.shape
    count = lax.axis_size("sp")
    dma = pltpu.SemaphoreType.DMA
    return pl.pallas_call(
        functools.partial(read_kernel, count),
        in_specs=[VMEM_SPEC] * 5,
        out_specs=VMEM_SPEC,
        out_shape=jax.ShapeDtypeStruct((rows, width), jnp.bfloat16),
        scratch_shapes=[
            pltpu.VMEM((2, count - 1) + maps.shape[1:], jnp.bfloat16),
            pltpu.VMEM((2, maps.shape[1], PAIR, PAIR), jnp.float32),
            dma((2, count - 1)),
            dma((2, count - 1)),
        ],
        compiler_params=pltpu.CompilerParams(collective_id=2, has_side_effects=True),
        cost_estimate=pl.CostEstimate(
            flops=8 * 4 * 2 * PAIR**3, bytes_accessed=40 << 20, transcendentals=0
        ),
    )(maps, ctx, reading, inside, gains.reshape(1, width))


def emit_kernel(
    tp_count,
    normed_ref,
    weight_ref,
    hidden_ref,
    gates_ref,
    out_ref,
    product_ref,
    mate_ref,
    chip_ref,
    land_ref,
    mate_send,
    mate_recv,
    chip_send,
    chip_recv,
    mixed_ref,
    token_ref,
    token_send,
    token_recv,
):
    tp_own, sp_own = lax.axis_index("tp"), lax.axis_index("sp")
    chips = tp_count // 2
    chip, core = tp_own // 2, lax.rem(tp_own, 2)
    mate = {"tp": chip * 2 + 1 - core}
    targets = [{"tp": lax.rem(chip + step, chips) * 2 + core} for step in range(1, chips)]
    pieces = product_ref.shape[0]
    token_peers = others("sp", pieces)
    greet([mate] + targets + token_peers)
    span = product_ref.shape[4]
    height = out_ref.shape[0]
    mate_copies = []
    for piece in range(pieces):
        step = (piece + 1) % pieces
        block = jnp.dot(
            normed_ref[lax.rem(sp_own + step, pieces)],
            weight_ref[...],
            preferred_element_type=jnp.float32,
        ).astype(jnp.bfloat16)
        for place in range(chips):
            for side in range(2):
                first = (place * 2 + side) * height
                product_ref[piece, side, place] = block[first : first + height]
        copy = remote(
            product_ref.at[piece, 1 - core],
            mate_ref.at[piece],
            mate_send.at[piece],
            mate_recv.at[piece],
            mate,
        )
        copy.start()
        mate_copies.append(copy)
    chip_copies = []
    for piece in range(pieces):
        mate_copies[piece].wait_recv()
        summed = product_ref[piece, core].astype(jnp.float32) + mate_ref[piece].astype(
            jnp.float32
        )
        chip_ref[piece] = summed.astype(jnp.bfloat16)
        for step, target in enumerate(targets):
            copy = remote(
                chip_ref.at[piece, lax.rem(chip + step + 1, chips)],
                land_ref.at[piece, step],
                chip_send.at[piece, step],
                chip_recv.at[piece, step],
                target,
            )
            copy.start()
            chip_copies.append(copy)
    token_copies = []
    for piece in range(pieces):
        mixed = product_ref[piece, core, chip].astype(jnp.float32) + mate_ref[
            piece, chip
        ].astype(jnp.float32)
        for step in range(chips - 1):
            chip_copies[piece * (chips - 1) + step].wait_recv()
            mixed += land_ref[piece, step].astype(jnp.float32)
        if piece < pieces - 1:
            mixed_ref[piece] = mixed.astype(jnp.bfloat16)
            copy = remote(
                mixed_ref.at[piece],
                token_ref.at[piece],
                token_send.at[piece],
                token_recv.at[piece],
                token_peers[piece],
            )
            copy.start()
            token_copies.append(copy)

    def finish(source, mixed):
        cols = pl.ds(pl.multiple_of(source * span, PAIR), span)
        out_ref[:, cols] = (
            hidden_ref[:, cols].astype(jnp.float32) + gates_ref[:, cols] * mixed
        ).astype(out_ref.dtype)

    finish(sp_own, mixed)
    for piece, copy in enumerate(token_copies):
        copy.wait_recv()
        source = lax.rem(sp_own + pieces - piece - 1, pieces)
        finish(source, token_ref[piece].astype(jnp.float32))
    for copy in mate_copies + chip_copies + token_copies:
        copy.wait_send()


def emit_call(normed, weight, hidden, gates):
    tp_count = lax.axis_size("tp")
    chips = tp_count // 2
    height, width = hidden.shape
    pieces = normed.shape[0]
    span = weight.shape[1]
    dma = pltpu.SemaphoreType.DMA
    vmem = lambda *shape: pltpu.VMEM(shape, jnp.bfloat16)
    return pl.pallas_call(
        functools.partial(emit_kernel, tp_count),
        in_specs=[VMEM_SPEC] * 4,
        out_specs=VMEM_SPEC,
        out_shape=jax.ShapeDtypeStruct(hidden.shape, jnp.bfloat16),
        scratch_shapes=[
            vmem(pieces, 2, chips, height, span),
            vmem(pieces, chips, height, span),
            vmem(pieces, chips, height, span),
            vmem(pieces, chips - 1, height, span),
            dma((pieces,)),
            dma((pieces,)),
            dma((pieces, chips - 1)),
            dma((pieces, chips - 1)),
            vmem(pieces - 1, height, span),
            vmem(pieces - 1, height, span),
            dma((pieces,)),
            dma((pieces,)),
        ],
        compiler_params=pltpu.CompilerParams(collective_id=3, has_side_effects=True),
    )(normed, weight, hidden, gates)


def body(
    hidden_items,
    sample_cond,
    prompt_items,
    prompt_cond,
    adjust_shifting,
    adjust_stretch,
    skip_valve,
    receiver_matrix,
    address_matrix,
    payload_matrix,
    joint_lower_projector,
    fading_raise_matrix,
    step_raise_matrix,
    feature_fading,
    spike_logfade,
    group_standard_factor,
    emit_matrix,
):
    span_rows = adjust_shifting.shape[0]
    conditions = jnp.stack([sample_cond, prompt_cond])
    activated = jax.nn.silu(conditions.astype(jnp.float32)).astype(jnp.bfloat16)
    own_cols = lax.dynamic_slice_in_dim(activated, lax.axis_index("sp") * span_rows, span_rows, 1)
    active = jnp.stack(
        [
            jnp.pad(own_cols, ((0, 14), (0, 0))),
            jnp.pad(own_cols, ((2, 12), (0, 0))),
            jnp.pad(own_cols[:1], ((4, 11), (0, 0))),
        ]
    )
    half = joint_lower_projector.shape[0] // 2
    down_own = jnp.concatenate(
        [joint_lower_projector[:half], joint_lower_projector[half:]], axis=1
    )
    features, ctx_mod, gates, down_all = front_call(
        active,
        adjust_shifting,
        adjust_stretch,
        skip_valve,
        hidden_items,
        prompt_items,
        down_own,
    )
    features = features.reshape(-1, hidden_items.shape[1])
    rank = joint_lower_projector.shape[1]
    down_weight = jnp.stack([down_all[:, :, :rank], down_all[:, :, rank:]], axis=1)
    down_weight = down_weight.reshape(-1, rank)
    ctx_key = stored(product(ctx_mod, address_matrix))
    ctx_value = stored(product(ctx_mod, payload_matrix))
    ctx_low = stored(product(ctx_mod, down_weight))
    ctx_joined = jnp.concatenate(
        [ctx_key, ctx_value, jnp.pad(ctx_low, ((0, 0), (0, PAIR - rank)))], axis=1
    )
    ctx_all = spread_call(ctx_joined, 1).reshape(-1, ctx_joined.shape[1])
    maps, ctx_state, reading, inside = chain_call(
        stored(product(features, receiver_matrix)),
        stored(product(features, address_matrix)),
        stored(product(features, payload_matrix)),
        stored(product(features, down_weight)),
        ctx_all,
        fading_raise_matrix,
        step_raise_matrix,
        feature_fading,
        spike_logfade,
    )
    normed = read_call(maps, ctx_state, reading, inside, group_standard_factor)
    return emit_call(spread_call(normed, 4), emit_matrix, hidden_items, gates)


def solution(mesh):
    placed = (
        P(("grp", "sp", "tp"), None),
        P("grp"),
        P(("grp", "sp"), None),
        P(),
        P("sp", "tp"),
        P("sp", "tp"),
        P("sp", "tp"),
        P(None, "tp"),
        P(None, "tp"),
        P(None, "tp"),
        P("sp", None),
        P(None, "tp"),
        P(None, "tp"),
        P("tp"),
        P(("grp", "sp"), "tp"),
        P("tp"),
        P("tp", "sp"),
    )
    return jax.shard_map(
        body, mesh=mesh, in_specs=placed, out_specs=P(("grp", "sp", "tp"), None), check_vma=False
    )
```
